32 devices in a mesh: ep: 8 (over z, y), tp: 4 (over x, core).
Axes of the slice: x: 2, y: 2, z: 4, core: 2. Of those that a mesh axis runs over, the one named last changes fastest.
Arguments:
- query_rows: bfloat16 [4096, 1024], P('ep', 'tp'), may hold values from -10 to 10
- key_rows: bfloat16 [4096, 1024], P('ep', 'tp'), may hold values from -10 to 10
- value_rows: bfloat16 [4096, 1024], P('ep', 'tp'), may hold values from -6 to 6
- key_bias: float32 [4096, 16], P(None, 'tp'), may hold values from -30 to 0
- out_weight: bfloat16 [1024, 2048], P('tp'), may hold values from -0.5625 to 0.5625
- moe_input: bfloat16 [4096, 2048], P(('ep', 'tp')), may hold values from -6 to 6
- moe_gain: float32 [2048], replicated, may hold values from 0.1 to 1.9
- expert_pick: int32 [4096, 2], P(('ep', 'tp')), may hold values from 0 to 7, as said below
- route_weight: float32 [4096, 2], P(('ep', 'tp')), may hold values from 0.1 to 1
- w_gate: bfloat16 [8, 2048, 1024], P('ep', None, 'tp'), may hold values from -0.125 to 0.125
- w_up: bfloat16 [8, 2048, 1024], P('ep', None, 'tp'), may hold values from -0.125 to 0.125
- w_down: bfloat16 [8, 1024, 2048], P('ep', 'tp'), may hold values from -0.1875 to 0.1875
Outputs:
- mixer_out: bfloat16 [4096, 2048], P(('ep', 'tp'))
- routed_out: bfloat16 [4096, 2048], P(('ep', 'tp'))
The draws below stay inside these ranges and needn't reach their ends.
Inputs may be any that keep to these rules, and one draw needn't show every extreme that they name: `expert_pick`: each row names two different experts of one group, expert e belonging to group e // 2; the rows of one device name no expert more than 64 times, and in every draw each expert of some group is named exactly 64 times by the rows of every device.
All inputs are finite; a program needn't handle non-finite values.
Results may differ from the reference program's by a relative error of at most 0.013.
Values may be sent and summed in bfloat16 or wider, within the bound.
A program may use at most 128 MiB of HBM per device.

```python
import math
import jax
import jax.numpy as jnp
from jax import lax

D = 2048
ATTENTION_HEADS = 16
HEAD_DIM = 64
FF = 1024
GROUPS = 4
TOPK = 2
SEQ_DEV = 512
TOK2_DEV = 128
EXPERTS = 8
FIRST_TOKENS1 = 4096
SEQ_BLOCKS = 8
TOKENS2 = 4096
CAP = 64
N_TP = 4


def draw_key_bias(key, part):
    flow_lanes = jax.random.split(jax.random.fold_in(key, 101), 5)
    fast_heads = jax.random.uniform(flow_lanes[0], (ATTENTION_HEADS,)) < 0.5
    jitter = jnp.clip(0.5 * jax.random.normal(flow_lanes[2], (FIRST_TOKENS1, ATTENTION_HEADS)), -1.0, 1.0)
    base_level = jnp.where(fast_heads, -jnp.log(4000.0), -jnp.log(130.0 * FIRST_TOKENS1))
    block_count = FIRST_TOKENS1 // SEQ_DEV
    shifts = jax.random.uniform(flow_lanes[1], (block_count, 1, ATTENTION_HEADS), minval=-0.75, maxval=0.75)
    shifts = jnp.broadcast_to(shifts, (block_count, SEQ_DEV, ATTENTION_HEADS)).reshape(FIRST_TOKENS1, ATTENTION_HEADS)
    bias_terms = base_level[None, :] + shifts + jitter
    slot_places = jax.random.randint(flow_lanes[3], (3, ATTENTION_HEADS), 0, FIRST_TOKENS1, dtype=jnp.int32)
    token_positions = jnp.arange(FIRST_TOKENS1, dtype=jnp.int32)[:, None]
    spike_mask = (token_positions == slot_places[0][None, :]) | (token_positions == slot_places[1][None, :]) | (token_positions == slot_places[2][None, :])
    spike_level = jax.random.uniform(flow_lanes[4], (FIRST_TOKENS1, ATTENTION_HEADS), minval=-2.0, maxval=-1.0)
    return jnp.where(spike_mask, spike_level, bias_terms).astype(jnp.float32)


def draw_expert_pick(key, part):
    base_key = jax.random.fold_in(key, 202)
    group_size = EXPERTS // GROUPS
    half_rows = TOK2_DEV // 2
    block_count = TOKENS2 // TOK2_DEV
    favored = jax.random.randint(jax.random.fold_in(base_key, 1), (), 0, GROUPS, dtype=jnp.int32)

    def one_block(block_key):
        flow_lanes = jax.random.split(block_key, 4)
        cut_points = jnp.sort(jax.random.randint(flow_lanes[0], (GROUPS - 2,), 0, half_rows + 1, dtype=jnp.int32))
        bounds = jnp.concatenate([jnp.zeros((1,), jnp.int32), cut_points, jnp.full((1,), half_rows, jnp.int32)])
        others = (favored + 1 + jnp.arange(GROUPS - 1, dtype=jnp.int32)) % GROUPS
        counts = jnp.zeros((GROUPS,), jnp.int32).at[favored].set(half_rows).at[others].set(bounds[1:] - bounds[:-1])
        group_ends = jnp.cumsum(counts)
        starts = group_ends - counts
        token_positions = jnp.arange(TOK2_DEV, dtype=jnp.int32)
        group_id = jnp.sum((token_positions[:, None] >= group_ends[None, :]).astype(jnp.int32), axis=1)
        group_rank = token_positions - starts[group_id]
        rotation = jax.random.randint(flow_lanes[1], (GROUPS,), 0, group_size, dtype=jnp.int32)
        offset = jax.random.randint(flow_lanes[2], (GROUPS,), 1, group_size, dtype=jnp.int32)
        first_pick = (group_rank + rotation[group_id]) % group_size
        second = (group_rank + rotation[group_id] + offset[group_id]) % group_size
        picked = jnp.stack([group_id * group_size + first_pick, group_id * group_size + second], axis=1)
        return picked[jax.random.permutation(flow_lanes[3], TOK2_DEV)]
    blocks = jax.vmap(one_block)(jax.random.split(base_key, block_count))
    return blocks.reshape(TOKENS2, TOPK).astype(jnp.int32)


def shard_levels(own_key, shape, cuts, least, top_value):
    gain = 1.0
    for dim, parts in cuts:
        heights = jax.random.uniform(jax.random.fold_in(jax.random.fold_in(own_key, 6), dim), (parts,), jnp.float32, least / len(cuts), top_value / len(cuts))
        gain = gain * jnp.repeat(jnp.exp(heights), shape[dim] // parts).reshape((-1,) + (1,) * (len(shape) - 1 - dim))
    return gain


def bell_draw(key, extent, spread, bound, shards=(), kind=jnp.bfloat16):
    drawn = jax.random.normal(key, extent, jnp.float32) * spread
    if len(shards) > 0:
        drawn = shard_levels(key, extent, shards, -0.22, 0.18) * drawn
    return jnp.clip(drawn, min=-bound, max=bound).astype(kind)


def setup_inputs(seed: int = 0) -> dict:
    keys = jax.random.split(jax.random.key(seed), 13)
    return {
        "query_rows": bell_draw(keys[0], (FIRST_TOKENS1, ATTENTION_HEADS * HEAD_DIM), 1.7, 10.0, ((0, 8), (1, 4))),
        "key_rows": bell_draw(keys[1], (FIRST_TOKENS1, ATTENTION_HEADS * HEAD_DIM), 1.7, 10.0, ((0, 8), (1, 4))),
        "value_rows": bell_draw(keys[2], (FIRST_TOKENS1, ATTENTION_HEADS * HEAD_DIM), 1.0, 6.0, ((0, 8), (1, 4))),
        "key_bias": draw_key_bias(jax.random.fold_in(keys[12], 71), 0),
        "out_weight": bell_draw(keys[4], (ATTENTION_HEADS * HEAD_DIM, D), (3.0 * (ATTENTION_HEADS * HEAD_DIM) ** -0.5), 0.5625, ((0, 4),)),
        "moe_input": bell_draw(keys[5], (TOKENS2, D), 1.0, 6.0, ((0, 32),)),
        "moe_gain": jnp.clip(1.0 + 0.18 * jax.random.normal(keys[6], (D,), jnp.float32), 0.1, 1.9),
        "expert_pick": draw_expert_pick(jax.random.fold_in(keys[12], 71), 0),
        "route_weight": jnp.clip(jnp.exp(math.log(1.0) - 2.3025851 * jax.random.uniform(keys[8], (TOKENS2, TOPK), jnp.float32) ** shard_levels(keys[8], (TOKENS2, TOPK), ((0, 32),), -0.2, 0.2)), 0.1, 1.0),
        "w_gate": bell_draw(keys[9], (EXPERTS, D, FF), D ** -0.5, 0.125, ((0, 8), (2, 4))),
        "w_up": bell_draw(keys[10], (EXPERTS, D, FF), D ** -0.5, 0.125, ((0, 8), (2, 4))),
        "w_down": bell_draw(keys[11], (EXPERTS, FF, D), FF ** -0.5, 0.1875, ((0, 8), (1, 4))),
    }


def block_values(query_heads, query_first, key_heads, value_heads, bias_heads, key_first, running):
    scores = jnp.einsum('hqd,hkd->hqk', query_heads.astype(jnp.float32), key_heads.astype(jnp.float32))
    scores = scores * HEAD_DIM ** (-0.5) + bias_heads[:, None, :]
    query_pos = query_first + jnp.arange(query_heads.shape[1], dtype=jnp.int32)
    key_pos = key_first + jnp.arange(key_heads.shape[1], dtype=jnp.int32)
    causal = (key_pos[None, :] < query_pos[:, None])[None]
    failure = jnp.where(causal, jax.nn.log_sigmoid(-scores), 0.0)
    remainder = lax.cumsum(failure, axis=2, reverse=True) - failure + running[:, :, None]
    stick_weight = jnp.where(causal, jnp.exp(jax.nn.log_sigmoid(scores) + remainder), 0.0).astype(jnp.bfloat16)
    portion = jnp.einsum('hqk,hkd->hqd', stick_weight.astype(jnp.float32), value_heads.astype(jnp.float32))
    return (portion, running + lax.optimization_barrier(jnp.sum(failure, axis=2)))

def mixer(query_rows, key_rows, value_rows, key_bias, out_weight):
    block_count = FIRST_TOKENS1 // SEQ_DEV

    def split_heads(rows):
        return jnp.transpose(rows.reshape(block_count, SEQ_DEV, ATTENTION_HEADS, HEAD_DIM), (0, 2, 1, 3))
    query_heads = split_heads(query_rows)
    key_heads = split_heads(key_rows)
    value_heads = split_heads(value_rows)
    bias_heads = jnp.transpose(key_bias.reshape(block_count, SEQ_DEV, ATTENTION_HEADS), (0, 2, 1))

    def one_block(block_index):

        def visit(step_index, carried):
            source = block_index - step_index
            portion, running = block_values(query_heads[block_index], block_index * SEQ_DEV, key_heads[source], value_heads[source], bias_heads[source], source * SEQ_DEV, carried[1])
            return (carried[0] + portion, running)
        start_state = (jnp.zeros((ATTENTION_HEADS, SEQ_DEV, HEAD_DIM), jnp.float32), jnp.zeros((ATTENTION_HEADS, SEQ_DEV), jnp.float32))
        steps_here = block_index % SEQ_BLOCKS + 1
        return lax.fori_loop(0, steps_here, visit, start_state)[0].astype(jnp.bfloat16)
    attended = lax.map(one_block, jnp.arange(block_count, dtype=jnp.int32))
    attended = jnp.transpose(attended, (0, 2, 1, 3)).reshape(FIRST_TOKENS1, ATTENTION_HEADS * HEAD_DIM)
    group_width = ATTENTION_HEADS * HEAD_DIM // N_TP
    summed = jnp.zeros((FIRST_TOKENS1, D), jnp.float32)
    for group in range(N_TP):
        columns = attended[:, group * group_width:(group + 1) * group_width]
        weights = out_weight[group * group_width:(group + 1) * group_width]
        rounded = jnp.dot(columns, weights, preferred_element_type=jnp.float32).astype(jnp.bfloat16)
        summed = summed + lax.optimization_barrier(rounded).astype(jnp.float32)
    return summed.astype(jnp.bfloat16)

def experts(moe_input, moe_gain, expert_pick, route_weight, w_gate, w_up, w_down):
    widened = moe_input.astype(jnp.float32)
    normed = (widened * lax.rsqrt(lax.optimization_barrier(jnp.mean(widened * widened, axis=1, keepdims=True)) + 1e-06) * moe_gain).astype(jnp.bfloat16)
    block_count = TOKENS2 // TOK2_DEV
    picks = expert_pick.reshape(block_count, TOK2_DEV * TOPK)
    matches = (picks[:, :, None] == jnp.arange(EXPERTS, dtype=jnp.int32)[None, None, :]).astype(jnp.int32)
    ranks = lax.optimization_barrier(jnp.sum((jnp.cumsum(matches, axis=1) - matches) * matches, axis=2))
    block_ids = jnp.arange(block_count, dtype=jnp.int32)[:, None]
    slots = picks * (block_count * CAP) + block_ids * CAP + ranks
    owners = block_ids * TOK2_DEV + jnp.arange(TOK2_DEV * TOPK, dtype=jnp.int32)[None, :] // TOPK
    table = jnp.full((EXPERTS * block_count * CAP,), TOKENS2, jnp.int32)
    table = table.at[slots.reshape(-1)].set(owners.reshape(-1)).reshape(EXPERTS, block_count * CAP)
    padded = jnp.concatenate([normed, jnp.zeros((1, D), jnp.bfloat16)], axis=0)

    def serve(expert):
        rows = padded[table[expert]]
        gate_in = jnp.dot(rows, w_gate[expert], preferred_element_type=jnp.float32)
        up_in = jnp.dot(rows, w_up[expert], preferred_element_type=jnp.float32)
        hidden = (jax.nn.silu(gate_in) * up_in).astype(jnp.bfloat16)
        return jnp.dot(hidden, w_down[expert], preferred_element_type=jnp.float32).astype(jnp.bfloat16)
    served = lax.map(serve, jnp.arange(EXPERTS, dtype=jnp.int32))
    chosen = served.reshape(EXPERTS * block_count * CAP, D)[slots.reshape(-1)]
    chosen = chosen.reshape(TOKENS2, TOPK, D).astype(jnp.float32)
    return lax.optimization_barrier(jnp.sum(chosen * route_weight[:, :, None], axis=1)).astype(jnp.bfloat16)

def reference(query_rows, key_rows, value_rows, key_bias, out_weight, moe_input, moe_gain, expert_pick, route_weight, w_gate, w_up, w_down):
    return (mixer(query_rows, key_rows, value_rows, key_bias, out_weight), experts(moe_input, moe_gain, expert_pick, route_weight, w_gate, w_up, w_down))
```

```python
import jax
import jax.numpy as jnp
from jax import lax
from jax.experimental import pallas as pl
from jax.experimental.pallas import tpu as pltpu
from jax.sharding import PartitionSpec as P

HEAD_DIM = 64
GROUPS = 4
TOPK = 2


norm_eps = 1e-06


def attend_kernel(tops_ref, query_ref, kv_ref, bias_ref, out_ref, acc_ref):
    tile = query_ref.shape[1]
    width = query_ref.shape[2]
    heads = width // HEAD_DIM
    slots = kv_ref.shape[0]
    per_block = kv_ref.shape[1] // tile
    top = tops_ref[pl.program_id(0)]
    own = tops_ref[2]
    turned = jnp.transpose(query_ref[0].astype(jnp.float32) * HEAD_DIM ** (-0.5))
    row_head = lax.broadcasted_iota(jnp.int32, (width, tile), 0) // HEAD_DIM
    queries = [jnp.where(row_head == h, turned, 0.0).astype(jnp.bfloat16) for h in range(heads)]
    key_at = lax.broadcasted_iota(jnp.int32, (tile, tile), 0)
    query_at = lax.broadcasted_iota(jnp.int32, (tile, tile), 1)
    causal = key_at < query_at
    later = jnp.where(causal, 1.0, 0.0).astype(jnp.bfloat16)
    acc_ref[...] = jnp.zeros_like(acc_ref)

    def visit(index, running, masked):
        block = index // per_block
        slot = lax.rem(own - block + slots, slots)
        rows = pl.ds(pl.multiple_of((index - block * per_block) * tile, tile), tile)
        first = pl.multiple_of(index * tile, tile)
        keys = kv_ref[slot, rows, :width]
        values = jnp.transpose(kv_ref[slot, rows, width:])
        passed = []
        for h in range(heads):
            scores = jnp.dot(keys, queries[h], preferred_element_type=jnp.float32)
            scores = scores + bias_ref[pl.ds(first, tile), h : h + 1]
            tail = jnp.log(1.0 + jnp.exp(-jnp.abs(scores)))
            lost = jnp.maximum(scores, 0.0) + tail
            won = jnp.minimum(scores, 0.0) - tail
            if masked:
                lost = jnp.where(causal, lost, 0.0)
            lost = lost.astype(jnp.bfloat16)
            after = jnp.dot(later, lost, preferred_element_type=jnp.float32)
            weight = jnp.exp(won - (after + running[h]))
            if masked:
                weight = jnp.where(causal, weight, 0.0)
            span = slice(h * HEAD_DIM, (h + 1) * HEAD_DIM)
            acc_ref[span, :] += jnp.dot(
                values[span, :], weight.astype(jnp.bfloat16), preferred_element_type=jnp.float32
            )
            passed.append(running[h] + after[0:1, :] + lost[0:1, :].astype(jnp.float32))
        return tuple(passed)

    running = tuple(jnp.zeros((1, tile), jnp.float32) for _ in range(heads))
    running = visit(top, running, True)
    lax.fori_loop(0, top, lambda step, carried: visit(top - 1 - step, carried, False), running)
    out_ref[0] = jnp.transpose(acc_ref[...]).astype(jnp.bfloat16)


def attend(tops, queries, kv, bias):
    parts, tile, width = queries.shape
    pairs = parts * tile * kv.shape[0] * kv.shape[1] * width // HEAD_DIM // 2
    return pl.pallas_call(
        attend_kernel,
        out_shape=jax.ShapeDtypeStruct(queries.shape, jnp.bfloat16),
        grid_spec=pltpu.PrefetchScalarGridSpec(
            num_scalar_prefetch=1,
            grid=(parts,),
            in_specs=[
                pl.BlockSpec((1, tile, width), lambda c, tops: (c, 0, 0)),
                pl.BlockSpec(memory_space=pltpu.VMEM),
                pl.BlockSpec(memory_space=pltpu.VMEM),
            ],
            out_specs=pl.BlockSpec((1, tile, width), lambda c, tops: (c, 0, 0)),
            scratch_shapes=[pltpu.VMEM((width, tile), jnp.float32)],
        ),
        cost_estimate=pl.CostEstimate(
            flops=pairs * 1000, bytes_accessed=kv.size * 2, transcendentals=pairs * 3
        ),
        compiler_params=pltpu.CompilerParams(vmem_limit_bytes=58 * 1024 * 1024),
    )(tops, queries, kv, bias)


def expand(arrived, gate_weights, up_weights):
    gate_in = jnp.einsum(
        "necm,emf->necf", arrived, gate_weights, preferred_element_type=jnp.float32
    )
    up_in = jnp.einsum("necm,emf->necf", arrived, up_weights, preferred_element_type=jnp.float32)
    return (jax.nn.silu(gate_in) * up_in).astype(jnp.bfloat16)


def contract(hidden, down_weights):
    return jnp.einsum("necf,efm->necm", hidden, down_weights, preferred_element_type=jnp.float32)


def local(
    query_rows,
    key_rows,
    value_rows,
    key_bias,
    out_weight,
    moe_input,
    moe_gain,
    expert_pick,
    route_weight,
    w_gate,
    w_up,
    w_down,
):
    block_rows = query_rows.shape[0]
    half_rows = block_rows // 2
    ep_index = lax.axis_index("ep")
    ep_count = lax.axis_size("ep")
    own_kv = jnp.concatenate([key_rows, value_rows], axis=1)
    mirror = [(i, ep_count - 1 - i) for i in range(ep_count)]
    far_query = lax.ppermute(query_rows[half_rows:], "ep", mirror)
    blocks = [own_kv]
    for shift in range(1, ep_count):
        pairs = [(i, (i + shift) % ep_count) for i in range(ep_count)]
        pairs = [(i, j) for i, j in pairs if i <= max(j, ep_count - 1 - j)]
        blocks.append(lax.ppermute(own_kv, "ep", pairs))
    tops = jnp.stack(
        [2 * ep_index, 2 * (ep_count - 1 - ep_index) + 1, ep_index]
    ).astype(jnp.int32)
    near, far = attend(
        tops, jnp.stack([query_rows[:half_rows], far_query]), jnp.stack(blocks), key_bias
    )
    attended = jnp.concatenate([near, lax.ppermute(far, "ep", mirror)], axis=0)
    mixer_out = lax.psum_scatter(
        jnp.dot(attended, out_weight, preferred_element_type=jnp.float32).astype(jnp.bfloat16),
        "tp",
        scatter_dimension=0,
        tiled=True,
    )
    token_count = moe_input.shape[0]
    widened = moe_input.astype(jnp.float32)
    normed = (
        widened
        * lax.rsqrt(jnp.mean(widened * widened, axis=1, keepdims=True) + norm_eps)
        * moe_gain
    ).astype(jnp.bfloat16)
    local_experts = w_gate.shape[0]
    expert_total = local_experts * ep_count
    capacity = GROUPS * token_count // expert_total
    picks = expert_pick.reshape(-1)
    matches = (picks[:, None] == jnp.arange(expert_total, dtype=jnp.int32)[None, :]).astype(
        jnp.int32
    )
    ranks = jnp.sum((jnp.cumsum(matches, axis=0) - matches) * matches, axis=1)
    slots = picks * capacity + ranks
    owners = jnp.arange(picks.shape[0], dtype=jnp.int32) // TOPK
    table = jnp.full((expert_total * capacity,), token_count, jnp.int32).at[slots].set(owners)
    padded = jnp.concatenate([normed, jnp.zeros((1, normed.shape[1]), jnp.bfloat16)], axis=0)
    outgoing = padded[table].reshape(ep_count, local_experts, capacity, normed.shape[1])
    arrived = lax.all_to_all(outgoing, "ep", split_axis=0, concat_axis=0, tiled=True)
    gate_all, up_all, down_all = (
        lax.all_gather(w_gate, "tp", axis=2, tiled=True),
        lax.all_gather(w_up, "tp", axis=2, tiled=True),
        lax.all_gather(w_down, "tp", axis=1, tiled=True),
    )
    served = contract(expand(arrived, gate_all, up_all), down_all).astype(jnp.bfloat16)
    returned = lax.all_to_all(served, "ep", split_axis=0, concat_axis=0, tiled=True)
    flat = returned.reshape(expert_total * capacity, returned.shape[3])
    chosen = flat[slots].reshape(token_count, TOPK, flat.shape[1]).astype(jnp.float32)
    routed_out = jnp.sum(chosen * route_weight[:, :, None], axis=1).astype(jnp.bfloat16)
    return (mixer_out, routed_out)


def solution(mesh):
    placed = (
        P("ep", "tp"),
        P("ep", "tp"),
        P("ep", "tp"),
        P(None, "tp"),
        P("tp", None),
        P(("ep", "tp"), None),
        P(),
        P(("ep", "tp"), None),
        P(("ep", "tp"), None),
        P("ep", None, "tp"),
        P("ep", None, "tp"),
        P("ep", "tp", None),
    )
    return jax.shard_map(
        local,
        mesh=mesh,
        in_specs=placed,
        out_specs=(P(("ep", "tp"), None), P(("ep", "tp"), None)),
        check_vma=False,
    )
```

```python
import jax
import jax.numpy as jnp
from jax import lax
from jax.experimental import pallas as pl
from jax.experimental.pallas import tpu as pltpu
from jax.sharding import PartitionSpec as P

HEAD_DIM = 64
GROUPS = 4
TOPK = 2
PAIR = 2


norm_eps = 1e-06


def attend_kernel(tops_ref, query_ref, bias_ref, *rest):
    block_refs = rest[:-4]
    out_ref, acc_ref, kv_ref, sems = rest[-4:]

    @pl.when(pl.program_id(0) == 0)
    def _():
        copies = [
            pltpu.make_async_copy(ref, kv_ref.at[slot], sems.at[slot])
            for slot, ref in enumerate(block_refs)
        ]
        for copy in copies:
            copy.start()
        for copy in copies:
            copy.wait()

    tile = query_ref.shape[1]
    width = query_ref.shape[2]
    heads = width // HEAD_DIM
    slots = kv_ref.shape[0]
    per_block = kv_ref.shape[1] // tile
    top = tops_ref[pl.program_id(0)]
    own = tops_ref[2]
    turned = jnp.transpose(query_ref[0].astype(jnp.float32) * HEAD_DIM ** (-0.5))
    row_head = lax.broadcasted_iota(jnp.int32, (width, tile), 0) // HEAD_DIM
    queries = [jnp.where(row_head == h, turned, 0.0).astype(jnp.bfloat16) for h in range(heads)]
    key_at = lax.broadcasted_iota(jnp.int32, (tile, tile), 0)
    query_at = lax.broadcasted_iota(jnp.int32, (tile, tile), 1)
    causal = key_at < query_at
    later = jnp.where(causal, 1.0, 0.0).astype(jnp.bfloat16)
    acc_ref[...] = jnp.zeros_like(acc_ref)

    def visit(index, running, masked):
        block = index // per_block
        away = lax.rem(own // PAIR - block // PAIR + slots // PAIR, slots // PAIR)
        slot = away * PAIR + lax.rem(own + block, PAIR)
        rows = pl.ds(pl.multiple_of((index - block * per_block) * tile, tile), tile)
        first = pl.multiple_of(index * tile, tile)
        keys = kv_ref[slot, rows, :width]
        values = jnp.transpose(kv_ref[slot, rows, width:])
        passed = []
        for h in range(heads):
            scores = jnp.dot(keys, queries[h], preferred_element_type=jnp.float32)
            scores = scores + bias_ref[pl.ds(first, tile), h : h + 1]
            tail = jnp.log(1.0 + jnp.exp(-jnp.abs(scores)))
            lost = jnp.maximum(scores, 0.0) + tail
            won = jnp.minimum(scores, 0.0) - tail
            if masked:
                lost = jnp.where(causal, lost, 0.0)
            lost = lost.astype(jnp.bfloat16)
            after = jnp.dot(later, lost, preferred_element_type=jnp.float32)
            weight = jnp.exp(won - (after + running[h]))
            if masked:
                weight = jnp.where(causal, weight, 0.0)
            span = slice(h * HEAD_DIM, (h + 1) * HEAD_DIM)
            acc_ref[span, :] += jnp.dot(
                values[span, :], weight.astype(jnp.bfloat16), preferred_element_type=jnp.float32
            )
            passed.append(running[h] + after[0:1, :] + lost[0:1, :].astype(jnp.float32))
        return tuple(passed)

    running = tuple(jnp.zeros((1, tile), jnp.float32) for _ in range(heads))
    running = visit(top, running, True)
    lax.fori_loop(0, top, lambda step, carried: visit(top - 1 - step, carried, False), running)
    out_ref[0] = jnp.transpose(acc_ref[...]).astype(jnp.bfloat16)


def attend(tops, queries, blocks, bias):
    parts, tile, width = queries.shape
    held = (len(blocks),) + blocks[0].shape
    pairs = parts * tile * held[0] * held[1] * width // HEAD_DIM // 2
    return pl.pallas_call(
        attend_kernel,
        out_shape=jax.ShapeDtypeStruct(queries.shape, jnp.bfloat16),
        grid_spec=pltpu.PrefetchScalarGridSpec(
            num_scalar_prefetch=1,
            grid=(parts,),
            in_specs=[
                pl.BlockSpec((1, tile, width), lambda c, tops: (c, 0, 0)),
                pl.BlockSpec(memory_space=pltpu.VMEM),
            ]
            + [pl.BlockSpec(memory_space=pl.ANY)] * len(blocks),
            out_specs=pl.BlockSpec((1, tile, width), lambda c, tops: (c, 0, 0)),
            scratch_shapes=[
                pltpu.VMEM((width, tile), jnp.float32),
                pltpu.VMEM(held, blocks[0].dtype),
                pltpu.SemaphoreType.DMA((len(blocks),)),
            ],
        ),
        cost_estimate=pl.CostEstimate(
            flops=pairs * 1000, bytes_accessed=len(blocks) * blocks[0].size * 2, transcendentals=pairs * 3
        ),
        compiler_params=pltpu.CompilerParams(vmem_limit_bytes=58 * 1024 * 1024),
    )(tops, queries, bias, *blocks)


def gather_blocks(own, count):
    ring = count // PAIR
    swap = [(i, i // PAIR * PAIR + (i + 1) % PAIR) for i in range(count)]
    ahead = [(i, (i + PAIR) % count) for i in range(count)]
    behind = [(j, i) for i, j in ahead]
    near = [own, lax.ppermute(own, "ep", swap)]
    far = {}
    for member in range(PAIR):
        reach = (ring - 1 + (member == 0)) // 2
        held = near[member]
        for step in range(1, reach + 1):
            held = lax.ppermute(held, "ep", ahead)
            far[step, member] = held
        held = near[member]
        for step in range(ring - 1, reach, -1):
            held = lax.ppermute(held, "ep", behind)
            far[step, member] = held
    return near + [far[step, member] for step in range(1, ring) for member in range(PAIR)]


def expand(arrived, gate_weights, up_weights):
    gate_in = jnp.einsum(
        "necm,emf->necf", arrived, gate_weights, preferred_element_type=jnp.float32
    )
    up_in = jnp.einsum("necm,emf->necf", arrived, up_weights, preferred_element_type=jnp.float32)
    return (jax.nn.silu(gate_in) * up_in).astype(jnp.bfloat16)


def contract(hidden, down_weights):
    return jnp.einsum("necf,efm->necm", hidden, down_weights, preferred_element_type=jnp.float32)


def local(
    query_rows,
    key_rows,
    value_rows,
    key_bias,
    out_weight,
    moe_input,
    moe_gain,
    expert_pick,
    route_weight,
    w_gate,
    w_up,
    w_down,
):
    block_rows = query_rows.shape[0]
    half_rows = block_rows // 2
    ep_index = lax.axis_index("ep")
    ep_count = lax.axis_size("ep")
    own_kv = jnp.concatenate([key_rows, value_rows], axis=1)
    mirror = [(i, ep_count - 1 - i) for i in range(ep_count)]
    far_query = lax.ppermute(query_rows[half_rows:], "ep", mirror)
    blocks = gather_blocks(own_kv, ep_count)
    tops = jnp.stack(
        [2 * ep_index, 2 * (ep_count - 1 - ep_index) + 1, ep_index]
    ).astype(jnp.int32)
    near, far = attend(
        tops, jnp.stack([query_rows[:half_rows], far_query]), blocks, key_bias
    )
    attended = jnp.concatenate([near, lax.ppermute(far, "ep", mirror)], axis=0)
    mixer_out = lax.psum_scatter(
        jnp.dot(attended, out_weight, preferred_element_type=jnp.float32).astype(jnp.bfloat16),
        "tp",
        scatter_dimension=0,
        tiled=True,
    )
    token_count = moe_input.shape[0]
    widened = moe_input.astype(jnp.float32)
    normed = (
        widened
        * lax.rsqrt(jnp.mean(widened * widened, axis=1, keepdims=True) + norm_eps)
        * moe_gain
    ).astype(jnp.bfloat16)
    local_experts = w_gate.shape[0]
    expert_total = local_experts * ep_count
    capacity = GROUPS * token_count // expert_total
    picks = expert_pick.reshape(-1)
    matches = (picks[:, None] == jnp.arange(expert_total, dtype=jnp.int32)[None, :]).astype(
        jnp.int32
    )
    ranks = jnp.sum((jnp.cumsum(matches, axis=0) - matches) * matches, axis=1)
    slots = picks * capacity + ranks
    owners = jnp.arange(picks.shape[0], dtype=jnp.int32) // TOPK
    table = jnp.full((expert_total * capacity,), token_count, jnp.int32).at[slots].set(owners)
    padded = jnp.concatenate([normed, jnp.zeros((1, normed.shape[1]), jnp.bfloat16)], axis=0)
    outgoing = padded[table].reshape(ep_count, local_experts, capacity, normed.shape[1])
    outgoing = lax.optimization_barrier((outgoing, far_query, *blocks))[0]
    arrived = lax.all_to_all(outgoing, "ep", split_axis=0, concat_axis=0, tiled=True)
    gate_all, up_all, down_all = (
        lax.all_gather(w_gate, "tp", axis=2, tiled=True),
        lax.all_gather(w_up, "tp", axis=2, tiled=True),
        lax.all_gather(w_down, "tp", axis=1, tiled=True),
    )
    served = contract(expand(arrived, gate_all, up_all), down_all).astype(jnp.bfloat16)
    returned = lax.all_to_all(served, "ep", split_axis=0, concat_axis=0, tiled=True)
    flat = returned.reshape(expert_total * capacity, returned.shape[3])
    chosen = flat[slots].reshape(token_count, TOPK, flat.shape[1]).astype(jnp.float32)
    routed_out = jnp.sum(chosen * route_weight[:, :, None], axis=1).astype(jnp.bfloat16)
    return (mixer_out, routed_out)


def solution(mesh):
    placed = (
        P("ep", "tp"),
        P("ep", "tp"),
        P("ep", "tp"),
        P(None, "tp"),
        P("tp", None),
        P(("ep", "tp"), None),
        P(),
        P(("ep", "tp"), None),
        P(("ep", "tp"), None),
        P("ep", None, "tp"),
        P("ep", None, "tp"),
        P("ep", "tp", None),
    )
    return jax.shard_map(
        local,
        mesh=mesh,
        in_specs=placed,
        out_specs=(P(("ep", "tp"), None), P(("ep", "tp"), None)),
        check_vma=False,
    )
```
